32 devices in a mesh: sp: 8 (over z, y), tp: 4 (over x, core).
Axes of the slice: x: 2, y: 2, z: 4, core: 2. Of those that a mesh axis runs over, the one named last changes fastest.
Arguments:
- queries: bfloat16 [8192, 1024], P('sp', 'tp'), may hold values from -300 to 300
- keys: bfloat16 [8192, 512], P('sp', 'tp'), may hold values from -6 to 6
- values: bfloat16 [8192, 512], P('sp', 'tp'), may hold values from -6 to 6
- sink_logits: float32 [16], P('tp'), may hold values from 1 to 6
- residual: bfloat16 [8192, 2048], P('sp'), may hold values from -3 to 3
- out_weight: bfloat16 [1024, 2048], P('tp'), may hold values from -0.5390625 to 0.5390625
- norm_gain: float32 [2048], replicated, may hold values from 0.1 to 1.9
- gate_weight: bfloat16 [2048, 5632], P('sp', 'tp'), may hold values from -0.125 to 0.125
- up_weight: bfloat16 [2048, 5632], P('sp', 'tp'), may hold values from -0.125 to 0.125
- down_weight: bfloat16 [2048, 5632], P('sp', 'tp'), may hold values from -0.1796875 to 0.1796875
Outputs:
- layer_out: bfloat16 [8192, 2048], P(('sp', 'tp'))
The draws below stay inside these ranges and needn't reach their ends.
All inputs are finite; a program needn't handle non-finite values.
Results may differ from the reference program's by a relative error of at most 0.02.
Values may be sent and summed in bfloat16 or wider, within the bound.
A program may use at most 64 MiB of HBM per device.

```python
import jax
import jax.numpy as jnp
from jax import lax

D = 2048
QH = 16
KVH = 8
HD = 64
FF = 5632
WINDOW = 128
TOKENS = 8192
GROUPS = 4


def shared_keys(key):
    base = jax.random.normal(jax.random.fold_in(key, 7), (TOKENS, KVH * HD), jnp.float32)
    base = jnp.clip(base, -6.0, 6.0)
    return base


def draw_keys(key, part):
    return shared_keys(key).astype(jnp.bfloat16)


def draw_queries(key, part):
    drawn = jax.random.normal(jax.random.fold_in(key, 13), (TOKENS, QH * HD), jnp.float32)
    drawn = jnp.clip(drawn, -6.0, 6.0)
    return drawn.astype(jnp.bfloat16)


def steps_of(own_key, extent, split, least, high):
    factor_of = 1.0
    for position, blocks in split:
        steps = jax.random.uniform(jax.random.fold_in(jax.random.fold_in(own_key, 6), position), (blocks,), jnp.float32, least / len(split), high / len(split))
        factor_of = factor_of * jnp.repeat(jnp.exp(steps), extent[position] // blocks).reshape((-1,) + (1,) * (len(extent) - 1 - position))
    return factor_of


def noise(rng, dims, scale, reach, cuts=(), kind=jnp.bfloat16):
    values = scale * jax.random.normal(rng, dims, jnp.float32)
    if cuts:
        values = values * steps_of(rng, dims, cuts, -0.22, 0.18)
    return jnp.clip(values, -reach, reach).astype(kind)


def setup_inputs(seed: int = 0) -> dict:
    seeds = jax.random.split(jax.random.key(seed), 11)
    queries = draw_queries(jax.random.fold_in(seeds[10], 71), 0)
    keys = draw_keys(jax.random.fold_in(seeds[10], 71), 0)
    values = noise(seeds[2], (TOKENS, KVH * HD), 1.0, 6.0, ((0, 8), (1, 4)))
    sink_logits = jnp.clip(1.0 + 5.0 * jax.random.uniform(seeds[3], (QH,), jnp.float32) ** steps_of(seeds[3], (QH,), ((0, 4),), -0.2, 0.2), 1.0, 6.0)
    residual = noise(seeds[4], (TOKENS, D), 0.5, 3.0, ((0, 8),))
    out_weight = noise(seeds[5], (QH * HD, D), 0.09, 0.5390625, ((0, 4),))
    norm_gain = jnp.clip(1.0 + 0.18 * jax.random.normal(seeds[6], (D,), jnp.float32), 0.1, 1.9)
    gate_weight = noise(seeds[7], (D, FF), D ** -0.5, 0.125, ((0, 8), (1, 4)))
    up_weight = noise(seeds[8], (D, FF), D ** -0.5, 0.125, ((0, 8), (1, 4)))
    down_weight = noise(seeds[9], (D, FF), 0.03, 0.1796875, ((0, 8), (1, 4)))
    return dict(queries=queries, keys=keys, values=values, sink_logits=sink_logits, residual=residual, out_weight=out_weight, norm_gain=norm_gain, gate_weight=gate_weight, up_weight=up_weight, down_weight=down_weight)


def attention_rows(queries, keys, values, sink_logits):
    total = queries.shape[0]
    blocks = total // WINDOW
    groups = QH // KVH
    query_blocks = queries.astype(jnp.float32).reshape(blocks, WINDOW, KVH, groups, HD)

    def banded(source):
        shaped = source.astype(jnp.float32).reshape(blocks, WINDOW, KVH, HD)
        earlier = jnp.concatenate([jnp.zeros_like(shaped[:1]), shaped[:-1]], axis=0)
        return jnp.concatenate([earlier, shaped], axis=1)
    key_band = banded(keys)
    value_band = banded(values)
    query_index = jnp.arange(WINDOW, dtype=jnp.int32)[:, None]
    key_index = jnp.arange(2 * WINDOW, dtype=jnp.int32)[None, :]
    distance = query_index - key_index + WINDOW
    key_place = jnp.arange(blocks, dtype=jnp.int32)[:, None, None] * WINDOW + key_index[None] - WINDOW
    valid = (distance >= 0) & (distance < WINDOW) & (key_place >= 0)
    head_number = jnp.arange(1, QH + 1, dtype=jnp.float32)
    slopes = (2.0 ** (-8.0 * head_number / QH)).reshape(KVH, groups, 1, 1, 1)
    scores = jnp.einsum('nqhgd,nkhd->hgnqk', query_blocks, key_band) * HD ** (-0.5)
    scores = scores - slopes * distance.astype(jnp.float32)
    scores = jnp.where(valid, scores, -jnp.inf)
    sinks = sink_logits.astype(jnp.float32).reshape(KVH, groups, 1, 1, 1)
    top = jnp.maximum(lax.optimization_barrier(jnp.max(scores, axis=-1, keepdims=True)), sinks)
    expd = jnp.exp(scores - top)
    denom = lax.optimization_barrier(jnp.sum(expd, axis=-1, keepdims=True)) + jnp.exp(sinks - top)
    weights = (expd / denom).astype(jnp.bfloat16)
    output = jnp.einsum('hgnqk,nkhd->nqhgd', weights.astype(jnp.float32), value_band)
    return output.reshape(total, QH * HD).astype(jnp.bfloat16)

def rounded(term):
    return lax.optimization_barrier(term.astype(jnp.bfloat16)).astype(jnp.float32)

def reference(queries, keys, values, sink_logits, residual, out_weight, norm_gain, gate_weight, up_weight, down_weight):
    attended = attention_rows(queries, keys, values, sink_logits)
    head_cols = QH * HD // GROUPS
    projected = jnp.zeros((queries.shape[0], D), jnp.float32)
    for group in range(GROUPS):
        term = jnp.dot(attended[:, group * head_cols:(group + 1) * head_cols], out_weight[group * head_cols:(group + 1) * head_cols], preferred_element_type=jnp.float32)
        projected = projected + rounded(term)
    mixed = (residual.astype(jnp.float32) + projected).astype(jnp.bfloat16)
    mixed_f = mixed.astype(jnp.float32)
    scale = lax.rsqrt(lax.optimization_barrier(jnp.mean(mixed_f * mixed_f, axis=-1, keepdims=True)) + 1e-06)
    normed = (mixed_f * scale * norm_gain.astype(jnp.float32)).astype(jnp.bfloat16)
    gate = jnp.dot(normed, gate_weight, preferred_element_type=jnp.float32)
    upper = jnp.dot(normed, up_weight, preferred_element_type=jnp.float32)
    hidden = (jax.nn.silu(gate) * upper).astype(jnp.bfloat16)
    unit_cols = FF // GROUPS
    expanded = jnp.zeros((queries.shape[0], D), jnp.float32)
    for group in range(GROUPS):
        term = lax.dot_general(hidden[:, group * unit_cols:(group + 1) * unit_cols], down_weight[:, group * unit_cols:(group + 1) * unit_cols], (((1,), (1,)), ((), ())), preferred_element_type=jnp.float32)
        expanded = expanded + rounded(term)
    return (mixed_f + 0.5 * expanded).astype(jnp.bfloat16)
```

```python
import functools

import jax
import jax.numpy as jnp
from jax import lax
from jax.experimental import pallas as pl
from jax.experimental.pallas import tpu as pltpu
from jax.sharding import PartitionSpec as P

QH = 16
HD = 64
WINDOW = 128
LAG = 2
GATE, UP, DOWN = 0, 1, 2
MESH = pl.DeviceIdType.MESH


def layer_kernel(
    zs,
    ys,
    tp,
    q_ref,
    k_ref,
    v_ref,
    sink_ref,
    res_hbm,
    ow_ref,
    gain_ref,
    gate_hbm,
    up_hbm,
    down_hbm,
    out_ref,
    weights,
    kext,
    vext,
    att,
    psend,
    precv,
    res,
    mixed,
    normed,
    hidden,
    esend,
    erecv,
    local_sem,
    halo_send,
    halo_recv,
    wsend,
    wrecv,
    rs_send,
    rs_recv,
    ag_send,
    ag_recv,
    ex_send,
    ex_recv,
):
    sp = zs * ys
    last = 2 * zs - 2
    me_sp = lax.axis_index("sp")
    me = lax.axis_index("tp")
    z = me_sp // ys
    y = me_sp % ys
    rows = q_ref.shape[0]
    own = rows // tp
    chunk = gate_hbm.shape[0]
    heads = q_ref.shape[1] // HD
    kvs = k_ref.shape[1] // HD
    groups = heads // kvs
    blocks = rows // WINDOW

    def block_rows(index, size):
        return pl.ds(pl.multiple_of(index * size, size), size)

    own_rows = block_rows(me, own)

    def piece(w, s, target, direction):
        part = weights.at[w, block_rows(s, chunk), :]
        return pltpu.make_async_remote_copy(
            src_ref=part,
            dst_ref=part,
            send_sem=wsend.at[w, s, direction],
            recv_sem=wrecv.at[w, s],
            device_id={"sp": target},
            device_id_type=MESH,
        )

    def offset(k):
        return ((k + 1) // 2) * (1 - 2 * (k % 2))

    def send_all(w, s, moves, drain):
        for condition, target, direction in moves:

            @pl.when(condition)
            def _():
                copy = piece(w, s, target, direction)
                if drain:
                    copy.wait_send()
                else:
                    copy.start()

    def zpart(k, ws, drain=False):
        off = offset(k)
        sz = z + off

        @pl.when((sz >= 0) & (sz < zs))
        def _():
            s = sz * ys + y
            for w in ws:
                if not drain:

                    @pl.when(k > 0)
                    def _():
                        piece(w, s, me_sp, 0).wait_recv()

                send_all(
                    w,
                    s,
                    (
                        ((off <= 0) & (z + 1 < zs), me_sp + ys, 0),
                        ((off >= 0) & (z >= 1), me_sp - ys, 1),
                        (y + 1 < ys, me_sp + 1, 2),
                        (y >= 1, me_sp - 1, 3),
                    ),
                    drain,
                )

    def ypart(k, ws, drain=False, then=None):
        sz = z + offset(k)

        @pl.when((sz >= 0) & (sz < zs))
        def _():
            for j in range(1, 2 * ys - 1):
                yoff = ((j + 1) // 2) * (1 - 2 * (j % 2))
                sy = y + yoff

                @pl.when((sy >= 0) & (sy < ys))
                def _():
                    s = sz * ys + sy
                    for w in ws:
                        if not drain:
                            piece(w, s, me_sp, 0).wait_recv()
                        if yoff < 0:
                            moves = ((y + 1 < ys, me_sp + 1, 2),)
                        else:
                            moves = ((y >= 1, me_sp - 1, 3),)
                        send_all(w, s, moves, drain)
                    if then is not None:
                        then(s)

    def loop(lo, hi, body):
        def step(k, carry):
            body(k)
            return carry

        lax.fori_loop(lo, hi, step, 0)

    locals_in = [
        pltpu.make_async_copy(
            source, weights.at[w, block_rows(me_sp, chunk), :], local_sem.at[w]
        )
        for w, source in enumerate((gate_hbm, up_hbm, down_hbm))
    ]
    res_in = pltpu.make_async_copy(res_hbm.at[own_rows, :], res, local_sem.at[3])
    for copy in locals_in:
        copy.start()
    res_in.start()

    def halo(i, source, target):
        return pltpu.make_async_remote_copy(
            src_ref=source.at[pl.ds(rows - WINDOW, WINDOW), :],
            dst_ref=target.at[pl.ds(0, WINDOW), :],
            send_sem=halo_send.at[i],
            recv_sem=halo_recv.at[i],
            device_id={"sp": me_sp + 1},
            device_id_type=MESH,
        )

    halos = ((0, k_ref, kext), (1, v_ref, vext))

    @pl.when(me_sp + 1 < sp)
    def _():
        for h in halos:
            halo(*h).start()

    locals_in[GATE].wait()
    locals_in[UP].wait()
    zpart(0, (GATE, UP))

    @pl.when(me_sp == 0)
    def _():
        kext[pl.ds(0, WINDOW), :] = jnp.zeros((WINDOW, kext.shape[1]), kext.dtype)
        vext[pl.ds(0, WINDOW), :] = jnp.zeros((WINDOW, vext.shape[1]), vext.dtype)

    kext[pl.ds(WINDOW, rows), :] = k_ref[...]
    vext[pl.ds(WINDOW, rows), :] = v_ref[...]
    qi = lax.broadcasted_iota(jnp.int32, (WINDOW, 2 * WINDOW), 0)
    ki = lax.broadcasted_iota(jnp.int32, (WINDOW, 2 * WINDOW), 1)
    distance = qi - ki + WINDOW
    distance_f = distance.astype(jnp.float32)
    in_window = (distance >= 0) & (distance < WINDOW)
    base_head = (me * heads).astype(jnp.float32)

    def attend(n):
        q_rows = block_rows(n, WINDOW)
        band = pl.ds(pl.multiple_of(n * WINDOW, WINDOW), 2 * WINDOW)
        place = me_sp * rows + n * WINDOW - WINDOW + ki
        valid = in_window & (place >= 0)
        outs = []
        for h in range(heads):
            kv = h // groups
            qh = q_ref[q_rows, h * HD : (h + 1) * HD]
            kh = kext[band, kv * HD : (kv + 1) * HD]
            vh = vext[band, kv * HD : (kv + 1) * HD]
            score = lax.dot_general(
                qh, kh, (((1,), (1,)), ((), ())), preferred_element_type=jnp.float32
            )
            exponent = jnp.full((1, 2 * WINDOW), base_head + (h + 1), jnp.float32)
            slope = jnp.exp2(exponent * (-8.0 / QH))
            score = score * HD ** (-0.5) - slope * distance_f
            score = jnp.where(valid, score, -jnp.inf)
            sink = sink_ref[h]
            top = jnp.maximum(jnp.max(score, axis=-1, keepdims=True), sink)
            expd = jnp.exp(score - top)
            denom = jnp.sum(expd, axis=-1, keepdims=True) + jnp.exp(sink - top)
            prob = (expd / denom).astype(jnp.bfloat16)
            outs.append(jnp.dot(prob, vh, preferred_element_type=jnp.float32))
        att[q_rows, :] = jnp.concatenate(outs, axis=1).astype(jnp.bfloat16)

    loop(1, blocks, attend)

    @pl.when(me_sp > 0)
    def _():
        for h in halos:
            halo(*h).wait_recv()

    attend(0)

    def to_owner(u):
        return pltpu.make_async_remote_copy(
            src_ref=psend.at[block_rows(u, own), :],
            dst_ref=precv.at[me],
            send_sem=rs_send.at[u],
            recv_sem=rs_recv.at[me],
            device_id={"tp": u},
            device_id_type=MESH,
        )

    def from_peer(t):
        return pltpu.make_async_remote_copy(
            src_ref=psend.at[own_rows, :],
            dst_ref=precv.at[t],
            send_sem=rs_send.at[t],
            recv_sem=rs_recv.at[t],
            device_id={"tp": t},
            device_id_type=MESH,
        )

    def project(j):
        u = (me + 1 + j) % tp
        u_rows = block_rows(u, own)
        psend[u_rows, :] = jnp.dot(
            att[u_rows, :], ow_ref[...], preferred_element_type=jnp.float32
        ).astype(jnp.bfloat16)

        @pl.when(j < tp - 1)
        def _():
            to_owner(u).start()

    loop(0, tp, project)

    def relay_gu(k):
        zpart(k, (GATE, UP))

        @pl.when(k >= LAG)
        def _():
            ypart(k - LAG, (GATE, UP))

    middle = min(5, last + 1)
    loop(1, middle, relay_gu)

    res_in.wait()
    for j in range(tp - 1):
        from_peer((me + 1 + j) % tp).wait_recv()
    tile = 32

    def norm_tile(i):
        t_rows = block_rows(i, tile)
        total = psend[pl.ds(pl.multiple_of(me * own + i * tile, tile), tile), :].astype(
            jnp.float32
        )
        for j in range(tp - 1):
            total = total + precv[(me + 1 + j) % tp, t_rows, :].astype(jnp.float32)
        mix = (res[t_rows, :].astype(jnp.float32) + total).astype(jnp.bfloat16)
        mixed[t_rows, :] = mix
        mix_f = mix.astype(jnp.float32)
        scale = lax.rsqrt(jnp.mean(mix_f * mix_f, axis=-1, keepdims=True) + 1e-06)
        normed[pl.ds(pl.multiple_of(me * own + i * tile, tile), tile), :] = (
            mix_f * scale * gain_ref[...]
        ).astype(jnp.bfloat16)

    loop(0, own // tile, norm_tile)

    def hand(block, peer):
        part = normed.at[block_rows(block, own), :]
        return pltpu.make_async_remote_copy(
            src_ref=part,
            dst_ref=part,
            send_sem=ag_send.at[peer],
            recv_sem=ag_recv.at[block],
            device_id={"tp": peer},
            device_id_type=MESH,
        )

    for j in range(tp - 1):
        hand(me, (me + 1 + j) % tp).start()

    loop(middle, last + 1, relay_gu)
    locals_in[DOWN].wait()
    zpart(0, (DOWN,))
    loop(last + 1 - LAG, last + 1, lambda k: ypart(k, (GATE, UP)))
    loop(1, 3, lambda k: zpart(k, (DOWN,)))

    def expand(j):
        u = (me + j) % tp

        @pl.when(j > 0)
        def _():
            hand(u, u).wait_recv()

        u_rows = block_rows(u, own)
        part = normed[u_rows, :]
        gate = jnp.dot(part, weights[GATE], preferred_element_type=jnp.float32)
        upper = jnp.dot(part, weights[UP], preferred_element_type=jnp.float32)
        hidden[u_rows, :] = (gate / (1.0 + jnp.exp(-gate)) * upper).astype(jnp.bfloat16)

    loop(0, tp, expand)

    def ex_copy(sender, u, s):
        return pltpu.make_async_remote_copy(
            src_ref=esend.at[s, block_rows(u, own), :],
            dst_ref=erecv.at[sender, s],
            send_sem=ex_send.at[u, s],
            recv_sem=ex_recv.at[sender, s],
            device_id={"tp": u},
            device_id_type=MESH,
        )

    def contract(s):
        block = weights[DOWN, block_rows(s, chunk), :]

        def one(j):
            u = (me + 1 + j) % tp
            u_rows = block_rows(u, own)
            esend[s, u_rows, :] = lax.dot_general(
                hidden[u_rows, :],
                block,
                (((1,), (1,)), ((), ())),
                preferred_element_type=jnp.float32,
            ).astype(jnp.bfloat16)

            @pl.when(j < tp - 1)
            def _():
                ex_copy(me, u, s).start()

        loop(0, tp, one)

    def relay_down(k):
        @pl.when((k >= 3) & (k <= last))
        def _():
            zpart(k, (DOWN,))

        sz = z + offset(k)

        @pl.when((k <= last) & (sz >= 0) & (sz < zs))
        def _():
            contract(sz * ys + y)

        @pl.when(k >= LAG)
        def _():
            ypart(k - LAG, (DOWN,), then=contract)

    loop(0, last + 1 + LAG, relay_down)

    for s in range(sp):
        cols = slice(s * chunk, (s + 1) * chunk)
        total = esend[s, own_rows, :].astype(jnp.float32)
        for j in range(tp - 1):
            t = (me + 1 + j) % tp
            ex_copy(t, t, s).wait_recv()
            total = total + erecv[t, s].astype(jnp.float32)
        out_ref[:, cols] = (mixed[:, cols].astype(jnp.float32) + 0.5 * total).astype(
            jnp.bfloat16
        )

    @pl.when(me_sp + 1 < sp)
    def _():
        for h in halos:
            halo(*h).wait_send()

    def drain(k):
        zpart(k, (GATE, UP, DOWN), drain=True)
        ypart(k, (GATE, UP, DOWN), drain=True)

    loop(0, last + 1, drain)

    def drain_peer(j):
        u = (me + 1 + j) % tp
        to_owner(u).wait_send()
        hand(me, u).wait_send()
        loop(0, sp, lambda s: ex_copy(me, u, s).wait_send())

    loop(0, tp - 1, drain_peer)


def per_device(
    zs,
    ys,
    tp,
    queries,
    keys,
    values,
    sink_logits,
    residual,
    out_weight,
    norm_gain,
    gate_weight,
    up_weight,
    down_weight,
):
    sp = zs * ys
    rows, width = residual.shape
    own = rows // tp
    chunk, units = gate_weight.shape
    vmem = pl.BlockSpec(memory_space=pltpu.VMEM)
    hbm = pl.BlockSpec(memory_space=pl.ANY)
    dma = pltpu.SemaphoreType.DMA
    bf16 = jnp.bfloat16
    return pl.pallas_call(
        functools.partial(layer_kernel, zs, ys, tp),
        out_shape=jax.ShapeDtypeStruct((own, width), bf16),
        in_specs=[
            vmem,
            vmem,
            vmem,
            pl.BlockSpec(memory_space=pltpu.SMEM),
            hbm,
            vmem,
            vmem,
            hbm,
            hbm,
            hbm,
        ],
        out_specs=vmem,
        scratch_shapes=[
            pltpu.VMEM((3, sp * chunk, units), bf16),
            pltpu.VMEM((rows + WINDOW, keys.shape[1]), bf16),
            pltpu.VMEM((rows + WINDOW, values.shape[1]), bf16),
            pltpu.VMEM((rows, queries.shape[1]), bf16),
            pltpu.VMEM((rows, width), bf16),
            pltpu.VMEM((tp, own, width), bf16),
            pltpu.VMEM((own, width), bf16),
            pltpu.VMEM((own, width), bf16),
            pltpu.VMEM((rows, width), bf16),
            pltpu.VMEM((rows, units), bf16),
            pltpu.VMEM((sp, rows, chunk), bf16),
            pltpu.VMEM((tp, sp, own, chunk), bf16),
            dma((4,)),
            dma((2,)),
            dma((2,)),
            dma((3, sp, 4)),
            dma((3, sp)),
            dma((tp,)),
            dma((tp,)),
            dma((tp,)),
            dma((tp,)),
            dma((tp, sp)),
            dma((tp, sp)),
        ],
        compiler_params=pltpu.CompilerParams(
            has_side_effects=True, vmem_limit_bytes=67_000_000
        ),
    )(
        queries,
        keys,
        values,
        sink_logits,
        residual,
        out_weight,
        norm_gain.reshape(1, width),
        gate_weight,
        up_weight,
        down_weight,
    )


def solution(mesh):
    tp = mesh.shape["tp"]
    sp = mesh.shape["sp"]
    ys = max(tp // 2, 1)
    if sp % ys:
        ys = 1
    return jax.shard_map(
        functools.partial(per_device, sp // ys, ys, tp),
        mesh=mesh,
        in_specs=(
            P("sp", "tp"),
            P("sp", "tp"),
            P("sp", "tp"),
            P("tp"),
            P("sp", None),
            P("tp", None),
            P(),
            P("sp", "tp"),
            P("sp", "tp"),
            P("sp", "tp"),
        ),
        out_specs=P(("sp", "tp"), None),
        check_vma=False,
    )
```

```python
import functools

import jax
import jax.numpy as jnp
from jax import lax
from jax.experimental import pallas as pl
from jax.experimental.pallas import tpu as pltpu
from jax.sharding import PartitionSpec as P

QH = 16
HD = 64
WINDOW = 128
LAG = 2
GATE, UP, DOWN_A, DOWN_B = 0, 1, 2, 3
MESH = pl.DeviceIdType.MESH


def layer_kernel(
    zs,
    ys,
    tp,
    halves,
    q_ref,
    k_ref,
    v_ref,
    sink_ref,
    res_hbm,
    ow_ref,
    gain_ref,
    gate_hbm,
    up_hbm,
    down_hbm,
    out_ref,
    weights,
    downs,
    kext,
    vext,
    att,
    psend,
    precv,
    res,
    mixed,
    normed,
    hidden,
    esend,
    erecv,
    local_sem,
    halo_send,
    halo_recv,
    wsend,
    wrecv,
    rs_send,
    rs_recv,
    ag_send,
    ag_recv,
    ex_send,
    ex_recv,
):
    sp = zs * ys
    last = 2 * zs - 2
    me_sp = lax.axis_index("sp")
    me = lax.axis_index("tp")
    z = me_sp // ys
    y = me_sp % ys
    rows = q_ref.shape[0]
    own = rows // tp
    chunk = gate_hbm.shape[0]
    half = chunk // halves
    split = halves == 2
    heads = q_ref.shape[1] // HD
    kvs = k_ref.shape[1] // HD
    groups = heads // kvs
    blocks = rows // WINDOW

    def block_rows(index, size):
        return pl.ds(pl.multiple_of(index * size, size), size)

    own_rows = block_rows(me, own)

    def part_of(w, s):
        if w >= DOWN_A:
            return downs.at[w - DOWN_A, block_rows(s, half), :]
        return weights.at[w, block_rows(s, chunk), :]

    def piece(w, s, target, direction):
        part = part_of(w, s)
        return pltpu.make_async_remote_copy(
            src_ref=part,
            dst_ref=part,
            send_sem=wsend.at[w, s, direction],
            recv_sem=wrecv.at[w, s],
            device_id={"sp": target},
            device_id_type=MESH,
        )

    def offset(k):
        return ((k + 1) // 2) * (1 - 2 * (k % 2))

    def send_all(w, s, moves, drain):
        for condition, target, direction in moves:

            @pl.when(condition)
            def _():
                copy = piece(w, s, target, direction)
                if drain:
                    copy.wait_send()
                else:
                    copy.start()

    def zpart(k, ws, drain=False):
        off = offset(k)
        sz = z + off

        @pl.when((sz >= 0) & (sz < zs))
        def _():
            s = sz * ys + y
            for w in ws:
                if not drain:

                    @pl.when(k > 0)
                    def _():
                        piece(w, s, me_sp, 0).wait_recv()

                send_all(
                    w,
                    s,
                    (
                        ((off <= 0) & (z + 1 < zs), me_sp + ys, 0),
                        ((off >= 0) & (z >= 1), me_sp - ys, 1),
                        (y + 1 < ys, me_sp + 1, 2),
                        (y >= 1, me_sp - 1, 3),
                    ),
                    drain,
                )

    def ypart(k, ws, drain=False, then=None):
        sz = z + offset(k)

        @pl.when((sz >= 0) & (sz < zs))
        def _():
            for j in range(1, 2 * ys - 1):
                yoff = ((j + 1) // 2) * (1 - 2 * (j % 2))
                sy = y + yoff

                @pl.when((sy >= 0) & (sy < ys))
                def _():
                    s = sz * ys + sy
                    for w in ws:
                        if not drain:
                            piece(w, s, me_sp, 0).wait_recv()
                        if yoff < 0:
                            moves = ((y + 1 < ys, me_sp + 1, 2),)
                        else:
                            moves = ((y >= 1, me_sp - 1, 3),)
                        send_all(w, s, moves, drain)
                    if then is not None:
                        then(s)

    def along_z(k, s, w, drain):
        off = offset(k)
        send_all(
            w,
            s,
            (
                ((off <= 0) & (z + 1 < zs), me_sp + ys, 0),
                ((off >= 0) & (z >= 1), me_sp - ys, 1),
            ),
            drain,
        )

    def yfirst(first, end, drain=False):
        for j in range(first, end):
            yoff = ((j + 1) // 2) * (1 - 2 * (j % 2))
            sy = y + yoff

            @pl.when((sy >= 0) & (sy < ys))
            def _():
                s = z * ys + sy
                if not drain and j > 0:
                    piece(DOWN_B, s, me_sp, 0).wait_recv()
                moves = ()
                if yoff <= 0:
                    moves += ((y + 1 < ys, me_sp + 1, 2),)
                if yoff >= 0:
                    moves += ((y >= 1, me_sp - 1, 3),)
                send_all(DOWN_B, s, moves, drain)

    def zsecond(k, drain=False):
        sz = z + offset(k)

        @pl.when((sz >= 0) & (sz < zs))
        def _():
            for sy in range(ys):
                s = sz * ys + sy
                if not drain:

                    @pl.when(k > 0)
                    def _():
                        piece(DOWN_B, s, me_sp, 0).wait_recv()

                along_z(k, s, DOWN_B, drain)

    def zdown(k):
        zpart(k, (DOWN_A,))
        if split:
            zsecond(k)

    def loop(lo, hi, body):
        def step(k, carry):
            body(k)
            return carry

        lax.fori_loop(lo, hi, step, 0)

    locals_in = [
        pltpu.make_async_copy(
            source, part_of(w, me_sp), local_sem.at[w]
        )
        for w, source in enumerate((gate_hbm, up_hbm))
    ] + [
        pltpu.make_async_copy(
            down_hbm.at[pl.ds(h * half, half), :],
            part_of(DOWN_A + h, me_sp),
            local_sem.at[DOWN_A + h],
        )
        for h in range(halves)
    ]
    res_in = pltpu.make_async_copy(res_hbm.at[own_rows, :], res, local_sem.at[4])
    for copy in locals_in:
        copy.start()
    res_in.start()

    def halo(i, source, target):
        return pltpu.make_async_remote_copy(
            src_ref=source.at[pl.ds(rows - WINDOW, WINDOW), :],
            dst_ref=target.at[pl.ds(0, WINDOW), :],
            send_sem=halo_send.at[i],
            recv_sem=halo_recv.at[i],
            device_id={"sp": me_sp + 1},
            device_id_type=MESH,
        )

    halos = ((0, k_ref, kext), (1, v_ref, vext))

    @pl.when(me_sp + 1 < sp)
    def _():
        for h in halos:
            halo(*h).start()

    locals_in[GATE].wait()
    locals_in[UP].wait()
    zpart(0, (GATE, UP))
    for h in range(halves):
        locals_in[DOWN_A + h].wait()
    if split:
        yfirst(0, 1)

    @pl.when(me_sp == 0)
    def _():
        kext[pl.ds(0, WINDOW), :] = jnp.zeros((WINDOW, kext.shape[1]), kext.dtype)
        vext[pl.ds(0, WINDOW), :] = jnp.zeros((WINDOW, vext.shape[1]), vext.dtype)

    kext[pl.ds(WINDOW, rows), :] = k_ref[...]
    vext[pl.ds(WINDOW, rows), :] = v_ref[...]
    qi = lax.broadcasted_iota(jnp.int32, (WINDOW, 2 * WINDOW), 0)
    ki = lax.broadcasted_iota(jnp.int32, (WINDOW, 2 * WINDOW), 1)
    distance = qi - ki + WINDOW
    distance_f = distance.astype(jnp.float32)
    in_window = (distance >= 0) & (distance < WINDOW)
    base_head = (me * heads).astype(jnp.float32)

    def attend(n):
        q_rows = block_rows(n, WINDOW)
        band = pl.ds(pl.multiple_of(n * WINDOW, WINDOW), 2 * WINDOW)
        place = me_sp * rows + n * WINDOW - WINDOW + ki
        valid = in_window & (place >= 0)
        outs = []
        for h in range(heads):
            kv = h // groups
            qh = q_ref[q_rows, h * HD : (h + 1) * HD]
            kh = kext[band, kv * HD : (kv + 1) * HD]
            vh = vext[band, kv * HD : (kv + 1) * HD]
            score = lax.dot_general(
                qh, kh, (((1,), (1,)), ((), ())), preferred_element_type=jnp.float32
            )
            exponent = jnp.full((1, 2 * WINDOW), base_head + (h + 1), jnp.float32)
            slope = jnp.exp2(exponent * (-8.0 / QH))
            score = score * HD ** (-0.5) - slope * distance_f
            score = jnp.where(valid, score, -jnp.inf)
            sink = sink_ref[h]
            top = jnp.maximum(jnp.max(score, axis=-1, keepdims=True), sink)
            expd = jnp.exp(score - top)
            denom = jnp.sum(expd, axis=-1, keepdims=True) + jnp.exp(sink - top)
            prob = (expd / denom).astype(jnp.bfloat16)
            outs.append(jnp.dot(prob, vh, preferred_element_type=jnp.float32))
        att[q_rows, :] = jnp.concatenate(outs, axis=1).astype(jnp.bfloat16)

    loop(1, blocks, attend)

    @pl.when(me_sp > 0)
    def _():
        for h in halos:
            halo(*h).wait_recv()

    attend(0)

    def to_owner(u):
        return pltpu.make_async_remote_copy(
            src_ref=psend.at[block_rows(u, own), :],
            dst_ref=precv.at[me],
            send_sem=rs_send.at[u],
            recv_sem=rs_recv.at[me],
            device_id={"tp": u},
            device_id_type=MESH,
        )

    def from_peer(t):
        return pltpu.make_async_remote_copy(
            src_ref=psend.at[own_rows, :],
            dst_ref=precv.at[t],
            send_sem=rs_send.at[t],
            recv_sem=rs_recv.at[t],
            device_id={"tp": t},
            device_id_type=MESH,
        )

    def project(j):
        u = (me + 1 + j) % tp
        u_rows = block_rows(u, own)
        psend[u_rows, :] = jnp.dot(
            att[u_rows, :], ow_ref[...], preferred_element_type=jnp.float32
        ).astype(jnp.bfloat16)

        @pl.when(j < tp - 1)
        def _():
            to_owner(u).start()

    loop(0, tp, project)

    def relay_gu(k):
        zpart(k, (GATE, UP))

        @pl.when(k >= LAG)
        def _():
            ypart(k - LAG, (GATE, UP))

    middle = min(5, last + 1)
    loop(1, middle, relay_gu)

    if split:
        yfirst(1, 2 * ys - 1)

    res_in.wait()
    for j in range(tp - 1):
        from_peer((me + 1 + j) % tp).wait_recv()
    tile = 32

    def norm_tile(i):
        t_rows = block_rows(i, tile)
        total = psend[pl.ds(pl.multiple_of(me * own + i * tile, tile), tile), :].astype(
            jnp.float32
        )
        for j in range(tp - 1):
            total = total + precv[(me + 1 + j) % tp, t_rows, :].astype(jnp.float32)
        mix = (res[t_rows, :].astype(jnp.float32) + total).astype(jnp.bfloat16)
        mixed[t_rows, :] = mix
        mix_f = mix.astype(jnp.float32)
        scale = lax.rsqrt(jnp.mean(mix_f * mix_f, axis=-1, keepdims=True) + 1e-06)
        normed[pl.ds(pl.multiple_of(me * own + i * tile, tile), tile), :] = (
            mix_f * scale * gain_ref[...]
        ).astype(jnp.bfloat16)

    loop(0, own // tile, norm_tile)

    def hand(block, peer):
        part = normed.at[block_rows(block, own), :]
        return pltpu.make_async_remote_copy(
            src_ref=part,
            dst_ref=part,
            send_sem=ag_send.at[peer],
            recv_sem=ag_recv.at[block],
            device_id={"tp": peer},
            device_id_type=MESH,
        )

    for j in range(tp - 1):
        hand(me, (me + 1 + j) % tp).start()

    loop(middle, last + 1, relay_gu)
    loop(0, 3, zdown)
    loop(last + 1 - LAG, last + 1, lambda k: ypart(k, (GATE, UP)))

    def expand(j):
        u = (me + j) % tp

        @pl.when(j > 0)
        def _():
            hand(u, u).wait_recv()

        @pl.when(j == tp // 2)
        def _():
            loop(3, 5, zdown)

        u_rows = block_rows(u, own)
        part = normed[u_rows, :]
        gate = jnp.dot(part, weights[GATE], preferred_element_type=jnp.float32)
        upper = jnp.dot(part, weights[UP], preferred_element_type=jnp.float32)
        hidden[u_rows, :] = (gate / (1.0 + jnp.exp(-gate)) * upper).astype(jnp.bfloat16)

    loop(0, tp, expand)

    def ex_copy(sender, u, s):
        return pltpu.make_async_remote_copy(
            src_ref=esend.at[s, block_rows(u, own), :],
            dst_ref=erecv.at[sender, s],
            send_sem=ex_send.at[u, s],
            recv_sem=ex_recv.at[sender, s],
            device_id={"tp": u},
            device_id_type=MESH,
        )

    def contract(h, sz):
        part = h * zs + sz
        block = downs[h, block_rows(sz, ys * half), :]

        def one(j):
            u = (me + 1 + j) % tp
            u_rows = block_rows(u, own)
            esend[part, u_rows, :] = lax.dot_general(
                hidden[u_rows, :],
                block,
                (((1,), (1,)), ((), ())),
                preferred_element_type=jnp.float32,
            ).astype(jnp.bfloat16)

            @pl.when(j < tp - 1)
            def _():
                ex_copy(me, u, part).start()

        loop(0, tp, one)

    def relay_down(k):
        @pl.when((k >= 5) & (k <= last))
        def _():
            zdown(k)

        if split:
            sz = z + offset(k)

            @pl.when((k <= last) & (sz >= 0) & (sz < zs))
            def _():
                contract(1, sz)

        @pl.when(k >= LAG)
        def _():
            ypart(k - LAG, (DOWN_A,))
            sy = z + offset(k - LAG)

            @pl.when((sy >= 0) & (sy < zs))
            def _():
                contract(0, sy)

    loop(0, last + 1 + LAG, relay_down)

    for part in range(halves * zs):
        h, sz = divmod(part, zs)
        total = esend[part, own_rows, :].astype(jnp.float32)
        for j in range(tp - 1):
            t = (me + 1 + j) % tp
            ex_copy(t, t, part).wait_recv()
            total = total + erecv[t, part].astype(jnp.float32)
        for sy in range(ys):
            first = (sz * ys + sy) * chunk + h * half
            cols = slice(first, first + half)
            out_ref[:, cols] = (
                mixed[:, cols].astype(jnp.float32)
                + 0.5 * total[:, sy * half : (sy + 1) * half]
            ).astype(jnp.bfloat16)

    @pl.when(me_sp + 1 < sp)
    def _():
        for h in halos:
            halo(*h).wait_send()

    def drain(k):
        zpart(k, (GATE, UP, DOWN_A), drain=True)
        ypart(k, (GATE, UP, DOWN_A), drain=True)
        if split:
            zsecond(k, drain=True)

    loop(0, last + 1, drain)
    if split:
        yfirst(0, 2 * ys - 1, drain=True)

    def drain_peer(j):
        u = (me + 1 + j) % tp
        to_owner(u).wait_send()
        hand(me, u).wait_send()
        loop(0, halves * zs, lambda s: ex_copy(me, u, s).wait_send())

    loop(0, tp - 1, drain_peer)


def per_device(
    zs,
    ys,
    tp,
    queries,
    keys,
    values,
    sink_logits,
    residual,
    out_weight,
    norm_gain,
    gate_weight,
    up_weight,
    down_weight,
):
    sp = zs * ys
    rows, width = residual.shape
    own = rows // tp
    chunk, units = gate_weight.shape
    halves = 2 if chunk % 256 == 0 else 1
    half = chunk // halves
    vmem = pl.BlockSpec(memory_space=pltpu.VMEM)
    hbm = pl.BlockSpec(memory_space=pl.ANY)
    dma = pltpu.SemaphoreType.DMA
    bf16 = jnp.bfloat16
    return pl.pallas_call(
        functools.partial(layer_kernel, zs, ys, tp, halves),
        out_shape=jax.ShapeDtypeStruct((own, width), bf16),
        in_specs=[
            vmem,
            vmem,
            vmem,
            pl.BlockSpec(memory_space=pltpu.SMEM),
            hbm,
            vmem,
            vmem,
            hbm,
            hbm,
            hbm,
        ],
        out_specs=vmem,
        scratch_shapes=[
            pltpu.VMEM((2, sp * chunk, units), bf16),
            pltpu.VMEM((halves, sp * half, units), bf16),
            pltpu.VMEM((rows + WINDOW, keys.shape[1]), bf16),
            pltpu.VMEM((rows + WINDOW, values.shape[1]), bf16),
            pltpu.VMEM((rows, queries.shape[1]), bf16),
            pltpu.VMEM((rows, width), bf16),
            pltpu.VMEM((tp, own, width), bf16),
            pltpu.VMEM((own, width), bf16),
            pltpu.VMEM((own, width), bf16),
            pltpu.VMEM((rows, width), bf16),
            pltpu.VMEM((rows, units), bf16),
            pltpu.VMEM((halves * zs, rows, ys * half), bf16),
            pltpu.VMEM((tp, halves * zs, own, ys * half), bf16),
            dma((5,)),
            dma((2,)),
            dma((2,)),
            dma((2 + halves, sp, 4)),
            dma((2 + halves, sp)),
            dma((tp,)),
            dma((tp,)),
            dma((tp,)),
            dma((tp,)),
            dma((tp, halves * zs)),
            dma((tp, halves * zs)),
        ],
        compiler_params=pltpu.CompilerParams(
            has_side_effects=True, vmem_limit_bytes=67_000_000
        ),
    )(
        queries,
        keys,
        values,
        sink_logits,
        residual,
        out_weight,
        norm_gain.reshape(1, width),
        gate_weight,
        up_weight,
        down_weight,
    )


def solution(mesh):
    tp = mesh.shape["tp"]
    sp = mesh.shape["sp"]
    ys = max(tp // 2, 1)
    if sp % ys:
        ys = 1
    return jax.shard_map(
        functools.partial(per_device, sp // ys, ys, tp),
        mesh=mesh,
        in_specs=(
            P("sp", "tp"),
            P("sp", "tp"),
            P("sp", "tp"),
            P("tp"),
            P("sp", None),
            P("tp", None),
            P(),
            P("sp", "tp"),
            P("sp", "tp"),
            P("sp", "tp"),
        ),
        out_specs=P(("sp", "tp"), None),
        check_vma=False,
    )
```

```python
import functools

import jax
import jax.numpy as jnp
from jax import lax
from jax.experimental import pallas as pl
from jax.experimental.pallas import tpu as pltpu
from jax.sharding import PartitionSpec as P

QH = 16
HD = 64
WINDOW = 128
LAG = 2
GATE, UP, DOWN_A, DOWN_B = 0, 1, 2, 3
MESH = pl.DeviceIdType.MESH


def layer_kernel(
    zs,
    ys,
    tp,
    halves,
    q_ref,
    k_ref,
    v_ref,
    sink_ref,
    res_hbm,
    ow_ref,
    gain_ref,
    gate_hbm,
    up_hbm,
    down_hbm,
    out_ref,
    weights,
    downs,
    kext,
    vext,
    att,
    psend,
    precv,
    res,
    mixed,
    normed,
    hidden,
    esend,
    erecv,
    local_sem,
    halo_send,
    halo_recv,
    wsend,
    wrecv,
    rs_send,
    rs_recv,
    ag_send,
    ag_recv,
    ex_send,
    ex_recv,
):
    sp = zs * ys
    last = 2 * zs - 2
    me_sp = lax.axis_index("sp")
    me = lax.axis_index("tp")
    z = me_sp // ys
    y = me_sp % ys
    rows = q_ref.shape[0]
    own = rows // tp
    chunk = gate_hbm.shape[0]
    half = chunk // halves
    split = halves == 2
    heads = q_ref.shape[1] // HD
    kvs = k_ref.shape[1] // HD
    groups = heads // kvs
    blocks = rows // WINDOW

    def block_rows(index, size):
        return pl.ds(pl.multiple_of(index * size, size), size)

    own_rows = block_rows(me, own)

    def part_of(w, s):
        if w >= DOWN_A:
            return downs.at[w - DOWN_A, block_rows(s, half), :]
        return weights.at[w, block_rows(s, chunk), :]

    def piece(w, s, target, direction):
        part = part_of(w, s)
        return pltpu.make_async_remote_copy(
            src_ref=part,
            dst_ref=part,
            send_sem=wsend.at[w, s, direction],
            recv_sem=wrecv.at[w, s],
            device_id={"sp": target},
            device_id_type=MESH,
        )

    def offset(k):
        return ((k + 1) // 2) * (1 - 2 * (k % 2))

    def send_all(w, s, moves, drain):
        for condition, target, direction in moves:

            @pl.when(condition)
            def _():
                copy = piece(w, s, target, direction)
                if drain:
                    copy.wait_send()
                else:
                    copy.start()

    def zpart(k, ws, drain=False):
        off = offset(k)
        sz = z + off

        @pl.when((sz >= 0) & (sz < zs))
        def _():
            s = sz * ys + y
            for w in ws:
                if not drain:

                    @pl.when(k > 0)
                    def _():
                        piece(w, s, me_sp, 0).wait_recv()

                send_all(
                    w,
                    s,
                    (
                        ((off <= 0) & (z + 1 < zs), me_sp + ys, 0),
                        ((off >= 0) & (z >= 1), me_sp - ys, 1),
                        (y + 1 < ys, me_sp + 1, 2),
                        (y >= 1, me_sp - 1, 3),
                    ),
                    drain,
                )

    def ypart(k, ws, drain=False, then=None):
        sz = z + offset(k)

        @pl.when((sz >= 0) & (sz < zs))
        def _():
            for j in range(1, 2 * ys - 1):
                yoff = ((j + 1) // 2) * (1 - 2 * (j % 2))
                sy = y + yoff

                @pl.when((sy >= 0) & (sy < ys))
                def _():
                    s = sz * ys + sy
                    for w in ws:
                        if not drain:
                            piece(w, s, me_sp, 0).wait_recv()
                        if yoff < 0:
                            moves = ((y + 1 < ys, me_sp + 1, 2),)
                        else:
                            moves = ((y >= 1, me_sp - 1, 3),)
                        send_all(w, s, moves, drain)
                    if then is not None:
                        then(s)

    def along_z(k, s, w, drain):
        off = offset(k)
        send_all(
            w,
            s,
            (
                ((off <= 0) & (z + 1 < zs), me_sp + ys, 0),
                ((off >= 0) & (z >= 1), me_sp - ys, 1),
            ),
            drain,
        )

    def yfirst(first, end, drain=False):
        for j in range(first, end):
            yoff = ((j + 1) // 2) * (1 - 2 * (j % 2))
            sy = y + yoff

            @pl.when((sy >= 0) & (sy < ys))
            def _():
                s = z * ys + sy
                if not drain and j > 0:
                    piece(DOWN_B, s, me_sp, 0).wait_recv()
                moves = ()
                if yoff <= 0:
                    moves += ((y + 1 < ys, me_sp + 1, 2),)
                if yoff >= 0:
                    moves += ((y >= 1, me_sp - 1, 3),)
                send_all(DOWN_B, s, moves, drain)

    def zsecond(k, drain=False):
        sz = z + offset(k)

        @pl.when((sz >= 0) & (sz < zs))
        def _():
            for sy in range(ys):
                s = sz * ys + sy
                if not drain:

                    @pl.when(k > 0)
                    def _():
                        piece(DOWN_B, s, me_sp, 0).wait_recv()

                along_z(k, s, DOWN_B, drain)

    def zdown(k):
        zpart(k, (DOWN_A,))
        if split:
            zsecond(k)

    def loop(lo, hi, body):
        def step(k, carry):
            body(k)
            return carry

        lax.fori_loop(lo, hi, step, 0)

    locals_in = [
        pltpu.make_async_copy(
            source, part_of(w, me_sp), local_sem.at[w]
        )
        for w, source in enumerate((gate_hbm, up_hbm))
    ] + [
        pltpu.make_async_copy(
            down_hbm.at[pl.ds(h * half, half), :],
            part_of(DOWN_A + h, me_sp),
            local_sem.at[DOWN_A + h],
        )
        for h in range(halves)
    ]
    res_in = pltpu.make_async_copy(res_hbm.at[own_rows, :], res, local_sem.at[4])
    for copy in locals_in:
        copy.start()
    res_in.start()

    def halo(i, source, target):
        return pltpu.make_async_remote_copy(
            src_ref=source.at[pl.ds(rows - WINDOW, WINDOW), :],
            dst_ref=target.at[pl.ds(0, WINDOW), :],
            send_sem=halo_send.at[i],
            recv_sem=halo_recv.at[i],
            device_id={"sp": me_sp + 1},
            device_id_type=MESH,
        )

    halos = ((0, k_ref, kext), (1, v_ref, vext))

    @pl.when(me_sp + 1 < sp)
    def _():
        for h in halos:
            halo(*h).start()

    locals_in[GATE].wait()
    locals_in[UP].wait()
    zpart(0, (GATE, UP))
    for h in range(halves):
        locals_in[DOWN_A + h].wait()
    if split:
        yfirst(0, 1)

    @pl.when(me_sp == 0)
    def _():
        kext[pl.ds(0, WINDOW), :] = jnp.zeros((WINDOW, kext.shape[1]), kext.dtype)
        vext[pl.ds(0, WINDOW), :] = jnp.zeros((WINDOW, vext.shape[1]), vext.dtype)

    kext[pl.ds(WINDOW, rows), :] = k_ref[...]
    vext[pl.ds(WINDOW, rows), :] = v_ref[...]
    qi = lax.broadcasted_iota(jnp.int32, (WINDOW, 2 * WINDOW), 0)
    ki = lax.broadcasted_iota(jnp.int32, (WINDOW, 2 * WINDOW), 1)
    distance = qi - ki + WINDOW
    distance_f = distance.astype(jnp.float32)
    in_window = (distance >= 0) & (distance < WINDOW)
    base_head = (me * heads).astype(jnp.float32)

    def attend(n):
        q_rows = block_rows(n, WINDOW)
        band = pl.ds(pl.multiple_of(n * WINDOW, WINDOW), 2 * WINDOW)
        place = me_sp * rows + n * WINDOW - WINDOW + ki
        valid = in_window & (place >= 0)
        outs = []
        for h in range(heads):
            kv = h // groups
            qh = q_ref[q_rows, h * HD : (h + 1) * HD]
            kh = kext[band, kv * HD : (kv + 1) * HD]
            vh = vext[band, kv * HD : (kv + 1) * HD]
            score = lax.dot_general(
                qh, kh, (((1,), (1,)), ((), ())), preferred_element_type=jnp.float32
            )
            exponent = jnp.full((1, 2 * WINDOW), base_head + (h + 1), jnp.float32)
            slope = jnp.exp2(exponent * (-8.0 / QH))
            score = score * HD ** (-0.5) - slope * distance_f
            score = jnp.where(valid, score, -jnp.inf)
            sink = sink_ref[h]
            top = jnp.maximum(jnp.max(score, axis=-1, keepdims=True), sink)
            expd = jnp.exp(score - top)
            denom = jnp.sum(expd, axis=-1, keepdims=True) + jnp.exp(sink - top)
            prob = (expd / denom).astype(jnp.bfloat16)
            outs.append(jnp.dot(prob, vh, preferred_element_type=jnp.float32))
        att[q_rows, :] = jnp.concatenate(outs, axis=1).astype(jnp.bfloat16)

    loop(1, blocks, attend)

    @pl.when(me_sp > 0)
    def _():
        for h in halos:
            halo(*h).wait_recv()

    attend(0)

    def to_owner(u):
        return pltpu.make_async_remote_copy(
            src_ref=psend.at[block_rows(u, own), :],
            dst_ref=precv.at[me],
            send_sem=rs_send.at[u],
            recv_sem=rs_recv.at[me],
            device_id={"tp": u},
            device_id_type=MESH,
        )

    def from_peer(t):
        return pltpu.make_async_remote_copy(
            src_ref=psend.at[own_rows, :],
            dst_ref=precv.at[t],
            send_sem=rs_send.at[t],
            recv_sem=rs_recv.at[t],
            device_id={"tp": t},
            device_id_type=MESH,
        )

    def project(j):
        u = (me + 1 + j) % tp
        u_rows = block_rows(u, own)
        psend[u_rows, :] = jnp.dot(
            att[u_rows, :], ow_ref[...], preferred_element_type=jnp.float32
        ).astype(jnp.bfloat16)

        @pl.when(j < tp - 1)
        def _():
            to_owner(u).start()

    loop(0, tp, project)

    def relay_gu(k):
        zpart(k, (GATE, UP))

    middle = min(5, last + 1)
    loop(1, middle, relay_gu)

    if split:
        yfirst(1, 2 * ys - 1)

    res_in.wait()
    for j in range(tp - 1):
        from_peer((me + 1 + j) % tp).wait_recv()
    tile = 32

    def norm_tile(i):
        t_rows = block_rows(i, tile)
        total = psend[pl.ds(pl.multiple_of(me * own + i * tile, tile), tile), :].astype(
            jnp.float32
        )
        for j in range(tp - 1):
            total = total + precv[(me + 1 + j) % tp, t_rows, :].astype(jnp.float32)
        mix = (res[t_rows, :].astype(jnp.float32) + total).astype(jnp.bfloat16)
        mixed[t_rows, :] = mix
        mix_f = mix.astype(jnp.float32)
        scale = lax.rsqrt(jnp.mean(mix_f * mix_f, axis=-1, keepdims=True) + 1e-06)
        normed[pl.ds(pl.multiple_of(me * own + i * tile, tile), tile), :] = (
            mix_f * scale * gain_ref[...]
        ).astype(jnp.bfloat16)

    loop(0, own // tile, norm_tile)

    def hand(block, peer):
        part = normed.at[block_rows(block, own), :]
        return pltpu.make_async_remote_copy(
            src_ref=part,
            dst_ref=part,
            send_sem=ag_send.at[peer],
            recv_sem=ag_recv.at[block],
            device_id={"tp": peer},
            device_id_type=MESH,
        )

    for j in range(tp - 1):
        hand(me, (me + 1 + j) % tp).start()

    loop(middle, last + 1, relay_gu)
    loop(0, 3, zdown)
    loop(0, last + 1, lambda k: ypart(k, (GATE, UP)))

    def expand(j):
        u = (me + j) % tp

        @pl.when(j > 0)
        def _():
            hand(u, u).wait_recv()

        @pl.when(j == tp // 2)
        def _():
            loop(3, 5, zdown)

        u_rows = block_rows(u, own)
        part = normed[u_rows, :]
        gate = jnp.dot(part, weights[GATE], preferred_element_type=jnp.float32)
        upper = jnp.dot(part, weights[UP], preferred_element_type=jnp.float32)
        hidden[u_rows, :] = (gate / (1.0 + jnp.exp(-gate)) * upper).astype(jnp.bfloat16)

    loop(0, tp, expand)

    def ex_copy(sender, u, s):
        return pltpu.make_async_remote_copy(
            src_ref=esend.at[s, block_rows(u, own), :],
            dst_ref=erecv.at[sender, s],
            send_sem=ex_send.at[u, s],
            recv_sem=ex_recv.at[sender, s],
            device_id={"tp": u},
            device_id_type=MESH,
        )

    def contract(h, sz):
        part = h * zs + sz
        block = downs[h, block_rows(sz, ys * half), :]

        def one(j):
            u = (me + 1 + j) % tp
            u_rows = block_rows(u, own)
            esend[part, u_rows, :] = lax.dot_general(
                hidden[u_rows, :],
                block,
                (((1,), (1,)), ((), ())),
                preferred_element_type=jnp.float32,
            ).astype(jnp.bfloat16)

            @pl.when(j < tp - 1)
            def _():
                ex_copy(me, u, part).start()

        loop(0, tp, one)

    def relay_down(k):
        @pl.when((k >= 5) & (k <= last))
        def _():
            zdown(k)

        if split:
            sz = z + offset(k)

            @pl.when((k <= last) & (sz >= 0) & (sz < zs))
            def _():
                contract(1, sz)

        @pl.when(k >= LAG)
        def _():
            ypart(k - LAG, (DOWN_A,))
            sy = z + offset(k - LAG)

            @pl.when((sy >= 0) & (sy < zs))
            def _():
                contract(0, sy)

    loop(0, last + 1 + LAG, relay_down)

    for part in range(halves * zs):
        h, sz = divmod(part, zs)
        total = esend[part, own_rows, :].astype(jnp.float32)
        for j in range(tp - 1):
            t = (me + 1 + j) % tp
            ex_copy(t, t, part).wait_recv()
            total = total + erecv[t, part].astype(jnp.float32)
        for sy in range(ys):
            first = (sz * ys + sy) * chunk + h * half
            cols = slice(first, first + half)
            out_ref[:, cols] = (
                mixed[:, cols].astype(jnp.float32)
                + 0.5 * total[:, sy * half : (sy + 1) * half]
            ).astype(jnp.bfloat16)

    @pl.when(me_sp + 1 < sp)
    def _():
        for h in halos:
            halo(*h).wait_send()

    def drain(k):
        zpart(k, (GATE, UP, DOWN_A), drain=True)
        ypart(k, (GATE, UP, DOWN_A), drain=True)
        if split:
            zsecond(k, drain=True)

    loop(0, last + 1, drain)
    if split:
        yfirst(0, 2 * ys - 1, drain=True)

    def drain_peer(j):
        u = (me + 1 + j) % tp
        to_owner(u).wait_send()
        hand(me, u).wait_send()
        loop(0, halves * zs, lambda s: ex_copy(me, u, s).wait_send())

    loop(0, tp - 1, drain_peer)


def per_device(
    zs,
    ys,
    tp,
    queries,
    keys,
    values,
    sink_logits,
    residual,
    out_weight,
    norm_gain,
    gate_weight,
    up_weight,
    down_weight,
):
    sp = zs * ys
    rows, width = residual.shape
    own = rows // tp
    chunk, units = gate_weight.shape
    halves = 2 if chunk % 256 == 0 else 1
    half = chunk // halves
    vmem = pl.BlockSpec(memory_space=pltpu.VMEM)
    hbm = pl.BlockSpec(memory_space=pl.ANY)
    dma = pltpu.SemaphoreType.DMA
    bf16 = jnp.bfloat16
    return pl.pallas_call(
        functools.partial(layer_kernel, zs, ys, tp, halves),
        out_shape=jax.ShapeDtypeStruct((own, width), bf16),
        in_specs=[
            vmem,
            vmem,
            vmem,
            pl.BlockSpec(memory_space=pltpu.SMEM),
            hbm,
            vmem,
            vmem,
            hbm,
            hbm,
            hbm,
        ],
        out_specs=vmem,
        scratch_shapes=[
            pltpu.VMEM((2, sp * chunk, units), bf16),
            pltpu.VMEM((halves, sp * half, units), bf16),
            pltpu.VMEM((rows + WINDOW, keys.shape[1]), bf16),
            pltpu.VMEM((rows + WINDOW, values.shape[1]), bf16),
            pltpu.VMEM((rows, queries.shape[1]), bf16),
            pltpu.VMEM((rows, width), bf16),
            pltpu.VMEM((tp, own, width), bf16),
            pltpu.VMEM((own, width), bf16),
            pltpu.VMEM((own, width), bf16),
            pltpu.VMEM((rows, width), bf16),
            pltpu.VMEM((rows, units), bf16),
            pltpu.VMEM((halves * zs, rows, ys * half), bf16),
            pltpu.VMEM((tp, halves * zs, own, ys * half), bf16),
            dma((5,)),
            dma((2,)),
            dma((2,)),
            dma((2 + halves, sp, 4)),
            dma((2 + halves, sp)),
            dma((tp,)),
            dma((tp,)),
            dma((tp,)),
            dma((tp,)),
            dma((tp, halves * zs)),
            dma((tp, halves * zs)),
        ],
        compiler_params=pltpu.CompilerParams(
            has_side_effects=True, vmem_limit_bytes=67_000_000
        ),
    )(
        queries,
        keys,
        values,
        sink_logits,
        residual,
        out_weight,
        norm_gain.reshape(1, width),
        gate_weight,
        up_weight,
        down_weight,
    )


def solution(mesh):
    tp = mesh.shape["tp"]
    sp = mesh.shape["sp"]
    ys = max(tp // 2, 1)
    if sp % ys:
        ys = 1
    return jax.shard_map(
        functools.partial(per_device, sp // ys, ys, tp),
        mesh=mesh,
        in_specs=(
            P("sp", "tp"),
            P("sp", "tp"),
            P("sp", "tp"),
            P("tp"),
            P("sp", None),
            P("tp", None),
            P(),
            P("sp", "tp"),
            P("sp", "tp"),
            P("sp", "tp"),
        ),
        out_specs=P(("sp", "tp"), None),
        check_vma=False,
    )
```
